32 devices in a mesh: kv: 8 (over z, y), tp: 4 (over x, core).
Axes of the slice: x: 2, y: 2, z: 4, core: 2. Of those that a mesh axis runs over, the one named last changes fastest.
Arguments:
- queries: bfloat16 [6144, 2048], P('kv', 'tp'), may hold values from -6 to 6
- keys_values: bfloat16 [6144, 1024], P('kv', 'tp'), may hold values from -6 to 6
- log_sums: float32 [6144, 32], P('kv', 'tp'), may hold values from 6.5 to 7.5
- out_grad: bfloat16 [6144, 2048], P('kv', 'tp'), may hold values from -96 to 96
- inputs: bfloat16 [6144, 4096], P('kv'), may hold values from -0.046875 to 0.046875
- chosen: int32 [48, 16], P('kv'), may hold values from -1 to 95, as said below
Outputs:
- query_grad: bfloat16 [6144, 2048], P('kv', 'tp')
- kv_grad: float32 [6144, 1024], P('kv', 'tp')
- weight_grad: float32 [4096, 2048], P('kv', 'tp')
The draws below stay inside these ranges and needn't reach their ends.
Inputs may be any that keep to these rules, and one draw needn't show every extreme that they name: `chosen`: each row names distinct key blocks, none starting after the last position of that row's query block, and -1 in unused entries; at least half of 16 blocks are named where that many are allowed. From the query blocks of one index of kv, at most 6 distinct blocks of the 768 positions of any one index are named, and this most is reached on every index.
All inputs are finite; a program needn't handle non-finite values.
Results may differ from the reference program's by a relative error of at most 0.0051.
Values may be sent and summed in bfloat16 or wider, within the bound.
No kernel may reach another device: no remote copies, remote signals or barrier semaphores. Data moves between devices by JAX's collectives and lax.ppermute only.
A program may use at most 128 MiB of HBM per device.

```python
import jax
import jax.numpy as jnp
from jax import lax

D = 4096
H = 32
KVH = 8
DH = 64
BLK = 64
QB = 128
NSEL = 16
TOK_DEV = 768
TOKENS = 6144


def draw_chosen(key, part):
    device_count = TOKENS // TOK_DEV
    query_per = TOK_DEV // QB
    block_per = TOK_DEV // BLK
    block_total = TOKENS // BLK
    query_total = TOKENS // QB
    capacity = block_per // 2
    key_order, key_pop, key_jitter, key_count = jax.random.split(key, 4)
    order_keys = jax.random.randint(key_order, (device_count, device_count, block_per), 0, 1 << 16) * block_per + jnp.arange(block_per, dtype=jnp.int32)
    order_rank = jnp.argsort(jnp.argsort(order_keys, axis=-1, stable=True), axis=-1, stable=True)
    allowed = order_rank < capacity
    popular = jax.random.randint(key_pop, (device_count,), 0, 4)
    jitter = jax.random.randint(key_jitter, (query_total, block_total), 0, 1024)
    counts = jax.random.randint(key_count, (query_total,), NSEL // 2, NSEL + 1)
    block_ids = jnp.arange(block_total, dtype=jnp.int32)
    owner_dev = block_ids // block_per
    within = block_ids % block_per
    query_ids = jnp.arange(query_total, dtype=jnp.int32)
    device = query_ids // query_per
    local_blk = query_ids % query_per
    allow_rows = allowed[device[:, None], owner_dev[None, :], within[None, :]]
    first_rank = order_rank[device[:, None], owner_dev[None, :], within[None, :]] == 0
    causal = (block_ids * BLK)[None, :] <= (query_ids * QB + QB - 1)[:, None]
    eligible = allow_rows & causal & (owner_dev[None, :] <= device[:, None])
    last_block = (local_blk == query_per - 1)[:, None]
    own_dev = owner_dev[None, :] == device[:, None]
    before_dev = owner_dev[None, :] == device[:, None] - 1
    half_dev = owner_dev[None, :] == device[:, None] - device_count // 2
    forced = last_block & eligible & (own_dev | first_rank & (before_dev | half_dev))
    block_score = jitter + popular[owner_dev][None, :] * 1024 + forced.astype(jnp.int32) * 8192
    block_score = jnp.where(eligible, block_score, -1)
    composite = block_score * block_total + block_ids[None, :]
    top_values, top_blocks = lax.top_k(composite, NSEL)
    listed = (jnp.arange(NSEL, dtype=jnp.int32)[None, :] < counts[:, None]) & (top_values >= 0)
    return jnp.where(listed, top_blocks, -1).astype(jnp.int32)


def with_spikes(entries, key, source, target, blocks, factor):
    def block_of(dim):
        return (jnp.arange(entries.shape[dim]) // (entries.shape[dim] // blocks)).reshape((-1,) + (1,) * (entries.ndim - 1 - dim))

    near = jax.random.permutation(key, blocks)[block_of(target)]
    far = (block_of(target) + blocks // 2) % blocks
    return jnp.where((block_of(source) == near) | (block_of(source) == far), factor * entries, entries)


def block_scale(rng, shape, cuts, smallest, top_value):
    gain = 1.0
    for axis_at, shards_of in cuts:
        steps = jax.random.uniform(jax.random.fold_in(jax.random.fold_in(rng, 6), axis_at), (shards_of,), jnp.float32, smallest / len(cuts), top_value / len(cuts))
        gain = gain * jnp.repeat(jnp.exp(steps), shape[axis_at] // shards_of).reshape((-1,) + (1,) * (len(shape) - 1 - axis_at))
    return gain


def normal_values(own_key, extent, width, reach, cuts=(), kind=jnp.bfloat16):
    result = jax.random.normal(own_key, extent, jnp.float32) * width
    if len(cuts) > 0:
        result = block_scale(own_key, extent, cuts, -0.22, 0.18) * result
    return jnp.clip(result, min=-reach, max=reach).astype(kind)


def gaussian_with(rng, extent, spread, bound, shards, heavy, kind=jnp.bfloat16):
    values = spread * jax.random.normal(rng, extent, jnp.float32)
    if shards:
        values = values * block_scale(rng, extent, shards, -0.22, 0.18)
    return jnp.clip(with_spikes(values, jax.random.fold_in(rng, 3), *heavy), -bound, bound).astype(kind)


def setup_inputs(seed: int = 0) -> dict:
    key_list = jax.random.split(jax.random.key(seed), 7)
    return {
        "queries": normal_values(key_list[0], (TOKENS, H * DH), 1.0, 6.0, ((0, 8), (1, 4))),
        "keys_values": normal_values(key_list[1], (TOKENS, 2 * KVH * DH), 1.0, 6.0, ((0, 8), (1, 4))),
        "log_sums": jnp.clip(6.5 + 1.0 * jax.random.uniform(key_list[2], (TOKENS, H), jnp.float32) ** block_scale(key_list[2], (TOKENS, H), ((0, 8), (1, 4)), -0.2, 0.2), 6.5, 7.5),
        "out_grad": normal_values(key_list[3], (TOKENS, H * DH), 16.0, 96.0, ((0, 8), (1, 4))),
        "inputs": gaussian_with(key_list[4], (TOKENS, D), 0.0078125, 0.046875, ((0, 8),), (0, 1, 8, 2.0)),
        "chosen": draw_chosen(jax.random.fold_in(key_list[6], 71), 0),
    }


def reference(queries, keys_values, log_sums, out_grad, inputs, chosen):
    score_scale = DH ** -0.5
    group_size = H // KVH
    block_total = TOKENS // BLK
    row_width = 2 * KVH * DH
    kv_blocks = keys_values.reshape(block_total, BLK, KVH, 2, DH)

    def one_block(grad_table, block_index):
        row_start = block_index * QB
        query_blk = lax.dynamic_slice_in_dim(queries, row_start, QB, 0).astype(jnp.float32).reshape(QB, KVH, group_size, DH)
        grad_blk = lax.dynamic_slice_in_dim(out_grad, row_start, QB, 0).astype(jnp.float32).reshape(QB, KVH, group_size, DH)
        sums_blk = lax.dynamic_slice_in_dim(log_sums, row_start, QB, 0).reshape(QB, KVH, group_size)
        chosen_row = lax.dynamic_index_in_dim(chosen, block_index, 0, keepdims=False)
        present = chosen_row >= 0
        safe_row = jnp.maximum(chosen_row, 0).astype(jnp.int32)
        picked = kv_blocks[safe_row].astype(jnp.float32)
        key_blk = picked[:, :, :, 0, :].reshape(NSEL * BLK, KVH, DH)
        value_blk = picked[:, :, :, 1, :].reshape(NSEL * BLK, KVH, DH)
        key_pos = (safe_row[:, None] * BLK + jnp.arange(BLK, dtype=jnp.int32)[None, :]).reshape(-1)
        key_live = jnp.repeat(present, BLK)
        query_pos = row_start + jnp.arange(QB, dtype=jnp.int32)
        visible = key_live[None, :] & (key_pos[None, :] <= query_pos[:, None])
        scores = jnp.einsum('qhgd,nhd->qhgn', query_blk, key_blk) * score_scale
        attn_prob = jnp.where(visible[:, None, None, :], jnp.exp(scores - sums_blk[..., None]), jnp.float32(0.0))
        prob_round = lax.optimization_barrier(attn_prob.astype(jnp.bfloat16)).astype(jnp.float32)
        output = jnp.einsum('qhgn,nhd->qhgd', prob_round, value_blk)
        delta_row = jnp.sum(grad_blk * output, axis=-1)
        prob_grad = jnp.einsum('qhgd,nhd->qhgn', grad_blk, value_blk)
        score_grad = attn_prob * (prob_grad - delta_row[..., None])
        score_round = lax.optimization_barrier(score_grad.astype(jnp.bfloat16)).astype(jnp.float32)
        query_part = (score_scale * jnp.einsum('qhgn,nhd->qhgd', score_round, key_blk)).astype(jnp.bfloat16)
        key_part = score_scale * jnp.einsum('qhgn,qhgd->nhd', score_round, query_blk)
        value_part = jnp.einsum('qhgn,qhgd->nhd', prob_round, grad_blk)
        both_parts = jnp.stack([key_part, value_part], axis=2).reshape(NSEL, BLK, row_width)
        grad_table = grad_table.at[safe_row].add(both_parts)
        return grad_table, query_part.reshape(QB, H * DH)

    start_table = jnp.zeros((block_total, BLK, row_width), jnp.float32)
    grad_table, query_parts = lax.scan(one_block, start_table, jnp.arange(TOKENS // QB, dtype=jnp.int32))
    query_grad = query_parts.reshape(TOKENS, H * DH)
    kv_grad = grad_table.reshape(TOKENS, row_width)
    weight_grad = jnp.dot(inputs.T, query_grad, preferred_element_type=jnp.float32)
    return query_grad, kv_grad, weight_grad
```

```python
import functools

import jax
import jax.numpy as jnp
from jax import lax
from jax.experimental import pallas as pl
from jax.experimental.pallas import tpu as pltpu
from jax.sharding import PartitionSpec as P


DH = 64
BLK = 64
QB = 128
NSEL = 16
ROW = 2 * DH


def attn_kernel(chosen_ref, slot_ref, first_ref, q_ref, o_ref, lse_ref, kv_ref, dq_ref, tab_ref,
                x, xt, kvg, p_s, d_s, ds_s, acc, *, nsel, group, at, cb, scale):
    i = pl.program_id(0)
    cols = group * QB
    keys = nsel * BLK

    @pl.when(i == 0)
    def _():
        acc[...] = jnp.zeros_like(acc)
        x[...] = jnp.zeros_like(x)
        xt[...] = jnp.zeros_like(xt)

    q = q_ref[...] * jnp.bfloat16(scale)
    o = o_ref[...]
    qt, ot = q.T, o.T
    for a in range(group):
        s = slice(a * DH, (a + 1) * DH)
        r = pl.ds(a * QB, QB)
        r2 = pl.ds(cols + a * QB, QB)
        x[r, pl.ds(0, DH)] = q[:, s]
        x[r2, pl.ds(DH, DH)] = o[:, s]
        xt[pl.ds(0, DH), r] = qt[s]
        xt[pl.ds(DH, DH), r2] = ot[s]
    lse_t = lse_ref[at * group:(at + 1) * group, :]
    start = (first_ref[0] + i) * QB
    slots, limits = [], []
    for j in range(nsel):
        c = chosen_ref[i * nsel + j]
        slots.append(jnp.where(c >= 0, slot_ref[jnp.maximum(c, 0)], 0))
        limits.append(jnp.where(c >= 0, start - c * BLK, -(1 << 28)))
    rows = lax.broadcasted_iota(jnp.int32, (BLK, QB), 0)
    lanes = lax.broadcasted_iota(jnp.int32, (BLK, QB), 1)
    gap = rows - lanes
    for j in range(nsel):
        s = slots[j]
        kvg[pl.ds(j * BLK, BLK), :] = kv_ref[pl.ds(pl.multiple_of(s * BLK, BLK), BLK), :]
    pair = 2 * QB
    crow = cb * BLK
    for h in range(cols // pair):
        dsum = jnp.zeros((8, pair), jnp.float32)
        lse = jnp.concatenate([lse_t[2 * h:2 * h + 1], lse_t[2 * h + 1:2 * h + 2]], axis=1)
        for c in range(keys // crow):
            kv_c = kvg[pl.ds(c * crow, crow), :]
            st = jnp.dot(kv_c, xt[:, pl.ds(h * pair, pair)], preferred_element_type=jnp.float32)
            dp = jnp.dot(kv_c, xt[:, pl.ds(cols + h * pair, pair)], preferred_element_type=jnp.float32)
            for b in range(cb):
                lim = limits[c * cb + b]
                seen = gap <= lim
                seen = jnp.concatenate([seen, seen], axis=1)
                sl = slice(b * BLK, (b + 1) * BLK)
                p = jnp.where(seen, jnp.exp(st[sl] - lse), 0.0)
                d = dp[sl]
                prod = p.astype(jnp.bfloat16).astype(jnp.float32) * d
                dsum = dsum + jnp.sum(prod.reshape(BLK // 8, 8, pair), axis=0)
                r = pl.ds(c * crow + b * BLK, BLK)
                p_s[r, pl.ds(h * pair, pair)] = p
                d_s[r, pl.ds(h * pair, pair)] = d
        delta = jnp.sum(dsum, axis=0, keepdims=True)
        for c in range(keys // crow):
            r = pl.ds(c * crow, crow)
            p = p_s[r, pl.ds(h * pair, pair)]
            d = d_s[r, pl.ds(h * pair, pair)]
            ds_s[r, pl.ds(h * pair, pair)] = (p * (d - delta)).astype(jnp.bfloat16)
            ds_s[r, pl.ds(cols + h * pair, pair)] = p.astype(jnp.bfloat16)
    for c in range(keys // crow):
        g = jnp.dot(ds_s[pl.ds(c * crow, crow), :], x[...], preferred_element_type=jnp.float32)
        for b in range(cb):
            s = slots[c * cb + b]
            r = pl.ds(pl.multiple_of(s * BLK, BLK), BLK)
            acc[r, :] += g[b * BLK:(b + 1) * BLK]
    kt = kvg[...].T[:DH]
    dqt = jnp.dot(kt, ds_s[:, pl.ds(0, cols)], preferred_element_type=jnp.float32)
    stack = jnp.concatenate([dqt[:, a * QB:(a + 1) * QB] for a in range(group)], axis=0)
    dq_ref[...] = (scale * stack.T).astype(dq_ref.dtype)

    @pl.when(i == pl.num_programs(0) - 1)
    def _():
        tab_ref[...] = acc[...].astype(tab_ref.dtype)


def attn(chosen, slots, first, queries, out_grad, log_sums, kv, *, nsel, group, at, cb=4):
    nq = queries.shape[0] // QB
    cols = group * QB
    wide = pl.BlockSpec((QB, group * DH), lambda i, *_: (i, at))
    return pl.pallas_call(
        functools.partial(
            attn_kernel, nsel=nsel, group=group, at=at, cb=cb, scale=DH ** (-0.5)
        ),
        grid_spec=pltpu.PrefetchScalarGridSpec(
            num_scalar_prefetch=3,
            grid=(nq,),
            in_specs=[
                wide,
                wide,
                pl.BlockSpec((log_sums.shape[0], QB), lambda i, *_: (0, i)),
                pl.BlockSpec(kv.shape, lambda i, *_: (0, 0)),
            ],
            out_specs=[
                pl.BlockSpec((QB, group * DH), lambda i, *_: (i, 0)),
                pl.BlockSpec(kv.shape, lambda i, *_: (0, 0)),
            ],
            scratch_shapes=[
                pltpu.VMEM((2 * cols, ROW), jnp.bfloat16),
                pltpu.VMEM((ROW, 2 * cols), jnp.bfloat16),
                pltpu.VMEM((nsel * BLK, ROW), jnp.bfloat16),
                pltpu.VMEM((nsel * BLK, cols), jnp.float32),
                pltpu.VMEM((nsel * BLK, cols), jnp.float32),
                pltpu.VMEM((nsel * BLK, 2 * cols), jnp.bfloat16),
                pltpu.VMEM(kv.shape, jnp.float32),
            ],
        ),
        out_shape=[
            jax.ShapeDtypeStruct((nq * QB, group * DH), jnp.bfloat16),
            jax.ShapeDtypeStruct(kv.shape, jnp.bfloat16),
        ],
        compiler_params=pltpu.CompilerParams(dimension_semantics=("arbitrary",)),
        cost_estimate=pl.CostEstimate(
            flops=nq * nsel * BLK * ROW * cols * 10,
            bytes_accessed=4 * kv.size + 8 * nq * QB * group * DH,
            transcendentals=nq * nsel * BLK * cols,
        ),
        name="attn_bwd",
    )(chosen, slots, first, queries, out_grad, log_sums, kv)


def sum_kernel(ask_ref, *refs):
    out_ref = refs[-1]
    out_ref[...] = jnp.zeros_like(out_ref)
    entries = refs[0].shape[0] // BLK
    for g, ref in enumerate(refs[:-1]):
        for j in range(entries):
            a = ask_ref[j]

            @pl.when(a >= 0)
            def _(g=g, ref=ref, j=j, a=a):
                r = pl.ds(pl.multiple_of(a * BLK, BLK), BLK)
                add = ref[pl.ds(j * BLK, BLK), :].astype(jnp.float32)
                out_ref[r, pl.ds(g * ROW, ROW)] += add


def sum_blocks(asked, parts, tok_count):
    vmem = pl.BlockSpec(memory_space=pltpu.VMEM)
    return pl.pallas_call(
        sum_kernel,
        in_specs=[pl.BlockSpec(memory_space=pltpu.SMEM)] + [vmem] * len(parts),
        out_specs=vmem,
        out_shape=jax.ShapeDtypeStruct((tok_count, ROW * len(parts)), jnp.float32),
        name="sum_blocks",
    )(asked, *parts)


def pack_kernel(*refs):
    out_ref = refs[-1]
    n = refs[0].shape[0]
    for k, ref in enumerate(refs[:-1]):
        out_ref[pl.ds(k * n, n), :] = ref[...]


def pack(parts):
    vmem = pl.BlockSpec(memory_space=pltpu.VMEM)
    shape = (parts[0].shape[0] * len(parts), parts[0].shape[1])
    return pl.pallas_call(
        pack_kernel,
        in_specs=[vmem] * len(parts),
        out_specs=vmem,
        out_shape=jax.ShapeDtypeStruct(shape, parts[0].dtype),
        name="pack",
    )(*parts)


def weight_kernel(place_ref, *refs, near):
    quarters, parts = refs[:4], refs[4:4 + near]
    own_ref, other_ref, rows_t = refs[4 + near:]
    tok = parts[0].shape[0]
    for k in range(near):
        rows_t[:, pl.ds(k * tok, tok)] = parts[k][...].T
    core, chip = place_ref[0], place_ref[1]
    size = quarters[0].shape[1]
    for k in range(4):
        t = jnp.dot(rows_t[...], quarters[k][...], preferred_element_type=jnp.float32).T
        away = core if k < 2 else 1 - core
        sub = chip if k % 2 == 0 else 1 - chip
        at = pl.ds(pl.multiple_of(sub * size, size), size)

        @pl.when(away == 0)
        def _():
            own_ref[at, :] = t

        @pl.when(away == 1)
        def _():
            other_ref[at, :] = t.astype(other_ref.dtype)


def weight_parts(place, quarters, parts):
    vmem = pl.BlockSpec(memory_space=pltpu.VMEM)
    near = len(parts)
    tok, cols = parts[0].shape
    shape = (2 * quarters[0].shape[1], cols)
    flops = 2 * near * tok * cols * 2 * shape[0]
    return pl.pallas_call(
        functools.partial(weight_kernel, near=near),
        in_specs=[pl.BlockSpec(memory_space=pltpu.SMEM)] + [vmem] * (4 + near),
        out_specs=[vmem, vmem],
        out_shape=[
            jax.ShapeDtypeStruct(shape, jnp.float32),
            jax.ShapeDtypeStruct(shape, jnp.bfloat16),
        ],
        scratch_shapes=[pltpu.VMEM((cols, near * tok), jnp.bfloat16)],
        cost_estimate=pl.CostEstimate(
            flops=flops, bytes_accessed=2 * 5 * quarters[0].size, transcendentals=0
        ),
        name="weight_parts",
    )(place, *quarters, *parts)


def exchange(x):
    return lax.all_to_all(x, "kv", split_axis=0, concat_axis=0, tiled=True)


def hop(x, step, axis="kv"):
    n = lax.axis_size(axis)
    return lax.ppermute(x, axis, [(j, j ^ step) for j in range(n)])


def input_slices(inputs, near, far):
    tok = inputs.shape[0]
    width = inputs.shape[1] // (near * far)
    me, at = lax.axis_index("kv"), lax.axis_index("tp")
    here, core, chip = me % near, at % 2, (at // 2) % 2
    half = far // 2
    side = ((me // near) % 2) ^ core
    slices = []
    for step in range(near):
        parts = []
        for f in range(max(half // 2, 1)):
            owner = side * half + chip * (half // 2) + f
            col = (owner * near + (here ^ step)) * width
            if half == 1:
                parts.append(lax.dynamic_slice(inputs, (0, col + chip * (width // 2)), (tok, width // 2)))
            else:
                parts.append(lax.dynamic_slice(inputs, (0, col), (tok, width)))
        slices.append(parts[0] if len(parts) == 1 else jnp.concatenate(parts, axis=1))
    return slices


def shards(queries, keys_values, log_sums, out_grad, inputs, chosen):
    tok_count = queries.shape[0]
    heads_here = queries.shape[1] // DH
    kv_heads = keys_values.shape[1] // ROW
    group = heads_here // kv_heads
    blocks_here = tok_count // BLK
    query_blocks = tok_count // QB
    kv_count = lax.axis_size("kv")
    near = 4
    far = kv_count // near
    me = lax.axis_index("kv")
    first_block = me * query_blocks
    capacity = blocks_here // 2
    total_blocks = kv_count * blocks_here

    flat_ids = chosen.reshape(-1)
    needed = jnp.any(
        flat_ids[:, None] == jnp.arange(total_blocks, dtype=jnp.int32)[None, :], axis=0
    )
    needed = needed.reshape(kv_count, blocks_here).astype(jnp.int32)
    rank_in = jnp.cumsum(needed, axis=1) - 1
    matches = (needed[:, :, None] == 1) & (
        rank_in[:, :, None] == jnp.arange(capacity, dtype=jnp.int32)[None, None, :]
    )
    request = jnp.sum(
        matches.astype(jnp.int32) * jnp.arange(blocks_here, dtype=jnp.int32)[None, :, None], axis=1
    )
    request = jnp.where(jnp.any(matches, axis=1), request, -1)
    slices = input_slices(inputs, near, far)
    asked = exchange(request)
    asked, slices = lax.optimization_barrier((asked, slices))
    asked = asked.reshape(-1)
    slots = jnp.arange(kv_count, dtype=jnp.int32)[:, None] * capacity + rank_in
    slots = jnp.clip(slots, 0, kv_count * capacity - 1).reshape(-1)
    first = first_block.astype(jnp.int32).reshape(1)
    flat_chosen = chosen.reshape(-1)
    lse = log_sums.T

    sends = []
    local_blocks = keys_values.reshape(blocks_here, BLK, kv_heads * ROW)
    picked = local_blocks[jnp.maximum(asked, 0)]
    for g in range(kv_heads):
        sends.append(picked[:, :, g * ROW : (g + 1) * ROW].reshape(kv_count, capacity * BLK, ROW))

    got = [slices[0]]
    for step in range(1, near):
        got.append(hop(slices[step], step))
    tables = []
    for g in range(kv_heads):
        tables.append(exchange(sends[g]).reshape(kv_count * capacity * BLK, ROW))

    dqs, returned, sums = [], [], []
    nears = []
    for g in range(kv_heads):
        dq, tab = attn(
            flat_chosen, slots, first, queries, out_grad, lse, tables[g],
            nsel=NSEL, group=group, at=g,
        )
        dqs.append(dq)
        nears.append([dq])
        for step in range(1, near):
            nears[g].append(hop(dq, step))
        back = exchange(tab.reshape(kv_count, capacity * BLK, ROW))
        returned.append(back.reshape(kv_count * capacity * BLK, ROW))
    seen = pack(got)
    beside = hop(seen, 2, "tp")
    twin = hop(seen, 1, "tp")
    beside_twin = hop(beside, 1, "tp")
    quarters = (seen, beside, twin, beside_twin)
    at = lax.axis_index("tp").astype(jnp.int32)
    place = jnp.stack([at % 2, (at // 2) % 2])
    width = inputs.shape[1] // kv_count
    for g in range(kv_heads):
        own, other = weight_parts(place, quarters, nears[g])
        cols = own.shape[1]
        if far == 2:
            other = hop(other, near)
            sums.append(own + other.astype(jnp.float32))
        else:
            even = (me // near) % 2 == 0
            own = own.astype(jnp.bfloat16)
            parts = jnp.concatenate([jnp.where(even, own, other), jnp.where(even, other, own)], axis=0)
            parts = parts.reshape(far, width, cols)
            groups = [[d + f * near for f in range(far)] for d in range(near)]
            parts = lax.all_to_all(
                parts, "kv", split_axis=0, concat_axis=0, tiled=True, axis_index_groups=groups
            )
            sums.append(jnp.sum(parts.astype(jnp.float32), axis=0))
    query_grad = jnp.concatenate(dqs, axis=1)
    kv_grad = sum_blocks(asked, returned, tok_count)
    weight_grad = jnp.concatenate(sums, axis=1)
    return (query_grad, kv_grad, weight_grad)


def solution(mesh):
    in_specs = (
        P("kv", "tp"),
        P("kv", "tp"),
        P("kv", "tp"),
        P("kv", "tp"),
        P("kv", None),
        P("kv", None),
    )
    out_specs = (P("kv", "tp"), P("kv", "tp"), P("kv", "tp"))
    return jax.shard_map(shards, mesh=mesh, in_specs=in_specs, out_specs=out_specs, check_vma=False)
```

```python
import functools

import jax
import jax.numpy as jnp
from jax import lax
from jax.experimental import pallas as pl
from jax.experimental.pallas import tpu as pltpu
from jax.sharding import PartitionSpec as P


DH = 64
BLK = 64
QB = 128
NSEL = 16
ROW = 2 * DH


def attn_kernel(chosen_ref, slot_ref, first_ref, q_ref, o_ref, lse_ref, kv_ref, dq_ref, tab_ref,
                x, xt, kvg, p_s, d_s, ds_s, acc, *, nsel, group, at, unroll, scale):
    i = pl.program_id(0)
    cols = group * QB
    pair = 2 * QB

    @pl.when(i == 0)
    def _():
        acc[...] = jnp.zeros_like(acc)
        x[...] = jnp.zeros_like(x)
        xt[...] = jnp.zeros_like(xt)

    gap = lax.broadcasted_iota(jnp.int32, (BLK, QB), 0) - lax.broadcasted_iota(
        jnp.int32, (BLK, QB), 1
    )

    def prepare(u):
        q = q_ref[pl.ds(u * QB, QB), :] * jnp.bfloat16(scale)
        o = o_ref[pl.ds(u * QB, QB), :]
        qt, ot = q.T, o.T
        for a in range(group):
            s = slice(a * DH, (a + 1) * DH)
            r = pl.ds(a * QB, QB)
            r2 = pl.ds(cols + a * QB, QB)
            x[u, r, pl.ds(0, DH)] = q[:, s]
            x[u, r2, pl.ds(DH, DH)] = o[:, s]
            xt[u, pl.ds(0, DH), r] = qt[s]
            xt[u, pl.ds(DH, DH), r2] = ot[s]
        block = i * unroll + u
        start = (first_ref[0] + block) * QB
        slots, limits = [], []
        for j in range(nsel):
            c = chosen_ref[block * nsel + j]
            slots.append(jnp.where(c >= 0, slot_ref[jnp.maximum(c, 0)], 0))
            limits.append(jnp.where(c >= 0, start - c * BLK, -(1 << 28)))
        for j in range(nsel):
            r = pl.ds(pl.multiple_of(slots[j] * BLK, BLK), BLK)
            kvg[u, pl.ds(j * BLK, BLK), :] = kv_ref[r, :]
        return slots, limits

    def scores(u, h, limits):
        top = lse_ref[at * group + 2 * h:at * group + 2 * h + 1, pl.ds(u * QB, QB)]
        low_row = lse_ref[at * group + 2 * h + 1:at * group + 2 * h + 2, pl.ds(u * QB, QB)]
        lse = jnp.concatenate([top, low_row], axis=1)
        here = pl.ds(h * pair, pair)
        there = pl.ds(cols + h * pair, pair)
        st = jnp.dot(kvg[u], xt[u, :, here], preferred_element_type=jnp.float32)
        dp = jnp.dot(kvg[u], xt[u, :, there], preferred_element_type=jnp.float32)
        part = jnp.zeros((8, pair), jnp.float32)
        for j in range(nsel):
            seen = gap <= limits[j]
            seen = jnp.concatenate([seen, seen], axis=1)
            sl = slice(j * BLK, (j + 1) * BLK)
            p = jnp.where(seen, jnp.exp(st[sl] - lse), 0.0)
            d = dp[sl]
            low = p.astype(jnp.bfloat16)
            prod = low.astype(jnp.float32) * d
            part = part + jnp.sum(prod.reshape(BLK // 8, 8, pair), axis=0)
            r = pl.ds(j * BLK, BLK)
            p_s[u, r, here] = p
            d_s[u, r, here] = d
            ds_s[u, r, there] = low
        return jnp.sum(part, axis=0, keepdims=True)

    def grads(u, slots, deltas):
        for h in range(cols // pair):
            here = pl.ds(h * pair, pair)
            ds_s[u, :, here] = (p_s[u, :, here] * (d_s[u, :, here] - deltas[h])).astype(jnp.bfloat16)
        kt = kvg[u].T[:DH]
        dqt = jnp.dot(kt, ds_s[u, :, pl.ds(0, cols)], preferred_element_type=jnp.float32)
        g = jnp.dot(ds_s[u], x[u], preferred_element_type=jnp.float32)
        for j in range(nsel):
            r = pl.ds(pl.multiple_of(slots[j] * BLK, BLK), BLK)
            acc[r, :] += g[j * BLK:(j + 1) * BLK]
        stack = jnp.concatenate([dqt[:, a * QB:(a + 1) * QB] for a in range(group)], axis=0)
        dq_ref[pl.ds(u * QB, QB), :] = (scale * stack.T).astype(dq_ref.dtype)

    blocks = [prepare(u) for u in range(unroll)]
    deltas = [[scores(u, h, blocks[u][1]) for h in range(cols // pair)] for u in range(unroll)]
    for u in range(unroll):
        grads(u, blocks[u][0], deltas[u])

    @pl.when(i == pl.num_programs(0) - 1)
    def _():
        tab_ref[...] = acc[...].astype(tab_ref.dtype)


def attn(chosen, slots, first, queries, out_grad, log_sums, kv, *, nsel, group, at):
    nq = queries.shape[0] // QB
    unroll = next(u for u in (3, 2, 1) if nq % u == 0)
    cols = group * QB
    rows = unroll * QB
    wide = pl.BlockSpec((rows, group * DH), lambda i, *_: (i, at))
    return pl.pallas_call(
        functools.partial(
            attn_kernel, nsel=nsel, group=group, at=at, unroll=unroll, scale=DH ** (-0.5)
        ),
        grid_spec=pltpu.PrefetchScalarGridSpec(
            num_scalar_prefetch=3,
            grid=(nq // unroll,),
            in_specs=[
                wide,
                wide,
                pl.BlockSpec((log_sums.shape[0], rows), lambda i, *_: (0, i)),
                pl.BlockSpec(kv.shape, lambda i, *_: (0, 0)),
            ],
            out_specs=[
                pl.BlockSpec((rows, group * DH), lambda i, *_: (i, 0)),
                pl.BlockSpec(kv.shape, lambda i, *_: (0, 0)),
            ],
            scratch_shapes=[
                pltpu.VMEM((unroll, 2 * cols, ROW), jnp.bfloat16),
                pltpu.VMEM((unroll, ROW, 2 * cols), jnp.bfloat16),
                pltpu.VMEM((unroll, nsel * BLK, ROW), jnp.bfloat16),
                pltpu.VMEM((unroll, nsel * BLK, cols), jnp.float32),
                pltpu.VMEM((unroll, nsel * BLK, cols), jnp.float32),
                pltpu.VMEM((unroll, nsel * BLK, 2 * cols), jnp.bfloat16),
                pltpu.VMEM(kv.shape, jnp.float32),
            ],
        ),
        out_shape=[
            jax.ShapeDtypeStruct((nq * QB, group * DH), jnp.bfloat16),
            jax.ShapeDtypeStruct(kv.shape, jnp.bfloat16),
        ],
        compiler_params=pltpu.CompilerParams(dimension_semantics=("arbitrary",)),
        cost_estimate=pl.CostEstimate(
            flops=nq * nsel * BLK * ROW * cols * 10,
            bytes_accessed=4 * kv.size + 8 * nq * QB * group * DH,
            transcendentals=nq * nsel * BLK * cols,
        ),
        name="attn_bwd",
    )(chosen, slots, first, queries, out_grad, log_sums, kv)


def pick_kernel(ids_ref, own_ref, away_ref, out_ref):
    edge = own_ref.shape[0] // BLK
    for j in range(out_ref.shape[0] // BLK):
        at = jnp.maximum(ids_ref[j], 0)

        @pl.when(at < edge)
        def _(j=j, at=at):
            r = pl.ds(pl.multiple_of(at * BLK, BLK), BLK)
            out_ref[pl.ds(j * BLK, BLK), :] = own_ref[r, :]

        @pl.when(at >= edge)
        def _(j=j, at=at):
            r = pl.ds(pl.multiple_of((at - edge) * BLK, BLK), BLK)
            out_ref[pl.ds(j * BLK, BLK), :] = away_ref[r, :]


def pick_blocks(ids, own, away):
    vmem = pl.BlockSpec(memory_space=pltpu.VMEM)
    return pl.pallas_call(
        pick_kernel,
        in_specs=[pl.BlockSpec(memory_space=pltpu.SMEM), vmem, vmem],
        out_specs=vmem,
        out_shape=jax.ShapeDtypeStruct((ids.shape[0] * BLK, own.shape[1]), own.dtype),
        name="pick_blocks",
    )(ids, own, away)


def sum_kernel(ids_ref, in_ref, own_ref, away_ref, acc):
    edge = own_ref.shape[0]
    acc[...] = jnp.zeros_like(acc)
    for j in range(in_ref.shape[0] // BLK):
        at = ids_ref[j]

        @pl.when(at >= 0)
        def _(j=j, at=at):
            r = pl.ds(pl.multiple_of(at * BLK, BLK), BLK)
            acc[r, :] += in_ref[pl.ds(j * BLK, BLK), :].astype(jnp.float32)

    own_ref[...] = acc[pl.ds(0, edge), :]
    away_ref[...] = acc[pl.ds(edge, away_ref.shape[0]), :].astype(away_ref.dtype)


def sum_blocks(ids, back, own_rows, away_rows):
    vmem = pl.BlockSpec(memory_space=pltpu.VMEM)
    width = back.shape[1]
    return pl.pallas_call(
        sum_kernel,
        in_specs=[pl.BlockSpec(memory_space=pltpu.SMEM), vmem],
        out_specs=[vmem, vmem],
        out_shape=[
            jax.ShapeDtypeStruct((own_rows, width), jnp.float32),
            jax.ShapeDtypeStruct((away_rows, width), jnp.bfloat16),
        ],
        scratch_shapes=[pltpu.VMEM((own_rows + away_rows, width), jnp.float32)],
        name="sum_blocks",
    )(ids, back)


def pack_kernel(*refs):
    n = (len(refs) - 3)
    sources, out_ref = refs[:n], refs[n]
    buf, sems = refs[n + 1:]
    tok = buf.shape[1]
    ins = [pltpu.make_async_copy(sources[k], buf.at[k], sems.at[k]) for k in range(n)]
    outs = [
        pltpu.make_async_copy(buf.at[k], out_ref.at[pl.ds(k * tok, tok), :], sems.at[n + k])
        for k in range(n)
    ]
    for copy in ins:
        copy.start()
    for k in range(n):
        ins[k].wait()
        outs[k].start()
    for copy in outs:
        copy.wait()


def pack(parts):
    hbm = pl.BlockSpec(memory_space=pl.ANY)
    n = len(parts)
    shape = (parts[0].shape[0] * n, parts[0].shape[1])
    return pl.pallas_call(
        pack_kernel,
        in_specs=[hbm] * n,
        out_specs=hbm,
        out_shape=jax.ShapeDtypeStruct(shape, parts[0].dtype),
        scratch_shapes=[
            pltpu.VMEM((n,) + parts[0].shape, parts[0].dtype),
            pltpu.SemaphoreType.DMA((2 * n,)),
        ],
        name="pack",
    )(*parts)


def weight_kernel(place_ref, inputs_ref, *refs, near, pieces):
    sources = refs[:4 + near]
    own_ref, other_ref, rows_t, parts, quarters, sems = refs[4 + near:]
    tok = parts.shape[1]
    size = sources[0].shape[1]
    copies = [
        pltpu.make_async_copy(sources[4 + k], parts.at[k], sems.at[k]) for k in range(near)
    ]
    local, rest = [], []
    for k in range(4):
        for f in range(pieces):
            col = pl.ds(pl.multiple_of(place_ref[2 + k * pieces + f], 128), size // pieces)
            to = quarters.at[pl.ds(0, tok), pl.ds(k * size + f * (size // pieces), size // pieces)]
            at = near + 4 + k * pieces + f
            local.append(pltpu.make_async_copy(inputs_ref.at[:, col], to, sems.at[at]))
        to = quarters.at[pl.ds(tok, (near - 1) * tok), pl.ds(k * size, size)]
        rest.append(pltpu.make_async_copy(sources[k], to, sems.at[near + k]))
    for copy in copies:
        copy.start()
    for k in range(4):
        for copy in local[k * pieces:(k + 1) * pieces]:
            copy.start()
        rest[k].start()
    for k in range(near):
        copies[k].wait()
        rows_t[:, pl.ds(k * tok, tok)] = parts[k].T
    core, chip = place_ref[0], place_ref[1]
    for pair in range(2):
        for k in (2 * pair, 2 * pair + 1):
            rest[k].wait()
            for copy in local[k * pieces:(k + 1) * pieces]:
                copy.wait()
        both = jnp.dot(
            rows_t[...],
            quarters[:, pl.ds(pair * 2 * size, 2 * size)],
            preferred_element_type=jnp.float32,
        )
        away = core if pair == 0 else 1 - core
        for k in range(2):
            t = both[:, k * size:(k + 1) * size].T
            sub = chip if k == 0 else 1 - chip
            at = pl.ds(pl.multiple_of(sub * size, size), size)

            @pl.when(away == 0)
            def _(t=t, at=at):
                own_ref[at, :] = t

            @pl.when(away == 1)
            def _(t=t, at=at):
                other_ref[at, :] = t.astype(other_ref.dtype)


def weight_parts(place, inputs, quarters, parts):
    vmem = pl.BlockSpec(memory_space=pltpu.VMEM)
    near = len(parts)
    tok, cols = parts[0].shape
    size = quarters[0].shape[1]
    pieces = (place.shape[0] - 2) // 4
    flops = 2 * near * tok * cols * 4 * size
    return pl.pallas_call(
        functools.partial(weight_kernel, near=near, pieces=pieces),
        in_specs=[pl.BlockSpec(memory_space=pltpu.SMEM)]
        + [pl.BlockSpec(memory_space=pl.ANY)] * (5 + near),
        out_specs=[vmem, vmem],
        out_shape=[
            jax.ShapeDtypeStruct((2 * size, cols), jnp.float32),
            jax.ShapeDtypeStruct((2 * size, cols), jnp.bfloat16),
        ],
        scratch_shapes=[
            pltpu.VMEM((cols, near * tok), jnp.bfloat16),
            pltpu.VMEM((near, tok, cols), jnp.bfloat16),
            pltpu.VMEM((near * tok, 4 * size), jnp.bfloat16),
            pltpu.SemaphoreType.DMA((near + 4 + 4 * pieces,)),
        ],
        cost_estimate=pl.CostEstimate(
            flops=flops, bytes_accessed=2 * 6 * quarters[0].size, transcendentals=0
        ),
        name="weight_parts",
    )(place, inputs, *quarters, *parts)


def exchange(x, groups):
    return lax.all_to_all(
        x, "kv", split_axis=0, concat_axis=0, tiled=True, axis_index_groups=groups
    )


def hop(x, step, axis="kv"):
    n = lax.axis_size(axis)
    return lax.ppermute(x, axis, [(j, j ^ step) for j in range(n)])


def column_starts(width, near, far, here, core, chip):
    half = far // 2
    side = ((lax.axis_index("kv") // near) % 2) ^ core
    if half == 1:
        return [(side * near + here) * width + chip * (width // 2)], width // 2
    owners = [side * half + chip * (half // 2) + f for f in range(half // 2)]
    return [(owner * near + here) * width for owner in owners], width


def input_slices(inputs, near, far):
    tok = inputs.shape[0]
    width = inputs.shape[1] // (near * far)
    here, at = lax.axis_index("kv") % near, lax.axis_index("tp")
    slices = []
    for step in range(1, near):
        cols, size = column_starts(width, near, far, here ^ step, at % 2, (at // 2) % 2)
        parts = [lax.dynamic_slice(inputs, (0, col), (tok, size)) for col in cols]
        slices.append(parts[0] if len(parts) == 1 else jnp.concatenate(parts, axis=1))
    return slices


def shards(queries, keys_values, log_sums, out_grad, inputs, chosen):
    tok_count = queries.shape[0]
    heads_here = queries.shape[1] // DH
    kv_heads = keys_values.shape[1] // ROW
    group = heads_here // kv_heads
    blocks_here = tok_count // BLK
    query_blocks = tok_count // QB
    kv_count = lax.axis_size("kv")
    near = 4
    far = kv_count // near
    me = lax.axis_index("kv")
    first_block = me * query_blocks
    capacity = blocks_here // 2
    total_blocks = kv_count * blocks_here

    flat_ids = chosen.reshape(-1)
    needed = jnp.any(
        flat_ids[:, None] == jnp.arange(total_blocks, dtype=jnp.int32)[None, :], axis=0
    )
    needed = needed.reshape(kv_count, blocks_here).astype(jnp.int32)
    rank_in = jnp.cumsum(needed, axis=1) - 1
    matches = (needed[:, :, None] == 1) & (
        rank_in[:, :, None] == jnp.arange(capacity, dtype=jnp.int32)[None, None, :]
    )
    request = jnp.sum(
        matches.astype(jnp.int32) * jnp.arange(blocks_here, dtype=jnp.int32)[None, :, None], axis=1
    )
    request = jnp.where(jnp.any(matches, axis=1), request, -1)
    request = jnp.swapaxes(request.reshape(far, near, capacity), 0, 1)
    near_groups = [[f * near + d for d in range(near)] for f in range(far)]
    far_groups = [[f * near + d for f in range(far)] for d in range(near)]
    far_at = me // near

    slices = input_slices(inputs, near, far)
    heads_kv = [keys_values[:, g * ROW : (g + 1) * ROW] for g in range(kv_heads)]
    away_kv = []
    for g in range(kv_heads):
        if far == 2:
            away_kv.append(lax.ppermute(heads_kv[g], "kv", [(j, j + near) for j in range(near)]))
        else:
            away_kv.append(
                lax.all_gather(heads_kv[g], "kv", tiled=True, axis_index_groups=far_groups)
            )
    asked = exchange(request, near_groups)
    owner = jnp.arange(far, dtype=jnp.int32)
    offset = ((owner != far_at) if far == 2 else owner + 1).astype(jnp.int32) * blocks_here
    ids = jnp.where(asked >= 0, asked + offset[None, :, None], -1).reshape(-1)
    of_block = jnp.arange(total_blocks, dtype=jnp.int32) // blocks_here
    slots = ((of_block % near) * far + of_block // near) * capacity + rank_in.reshape(-1)
    slots = jnp.clip(slots, 0, kv_count * capacity - 1)
    first = first_block.astype(jnp.int32).reshape(1)
    flat_chosen = chosen.reshape(-1)
    lse = log_sums.T

    tables = []
    for g in range(kv_heads):
        send = pick_blocks(ids, heads_kv[g], away_kv[g])
        table = exchange(send.reshape(near, -1, ROW), near_groups)
        tables.append(table.reshape(kv_count * capacity * BLK, ROW))
    got = []
    for step in range(1, near):
        got.append(hop(slices[step - 1], step))

    dqs, returned, sums = [], [], []
    nears = []
    for g in range(kv_heads):
        dq, tab = attn(
            flat_chosen, slots, first, queries, out_grad, lse, tables[g],
            nsel=NSEL, group=group, at=g,
        )
        dqs.append(dq)
        nears.append([dq])
        for step in range(1, near):
            relay = g == kv_heads - 1 and step == 3
            nears[g].append(hop(nears[g][2], 1) if relay else hop(dq, step))
        back = exchange(tab.reshape(near, -1, ROW), near_groups)
        returned.append(back.reshape(kv_count * capacity * BLK, ROW))
    seen = pack(got)
    beside = hop(seen, 2, "tp")
    twin = hop(seen, 1, "tp")
    beside_twin = hop(beside, 1, "tp")
    quarters = (seen, beside, twin, beside_twin)
    at = lax.axis_index("tp").astype(jnp.int32)
    core, chip = at % 2, (at // 2) % 2
    width = inputs.shape[1] // kv_count
    entries = [core, chip]
    for k in range(4):
        cols, _ = column_starts(width, near, far, me % near, core ^ (k // 2), chip ^ (k % 2))
        entries += cols
    place = jnp.stack([jnp.asarray(e, jnp.int32) for e in entries])
    for g in range(kv_heads):
        own, other = weight_parts(place, inputs, quarters, nears[g])
        cols = own.shape[1]
        if far == 2:
            other = hop(other, near)
            sums.append(own + other.astype(jnp.float32))
        else:
            even = (me // near) % 2 == 0
            own = own.astype(jnp.bfloat16)
            parts = jnp.concatenate([jnp.where(even, own, other), jnp.where(even, other, own)], axis=0)
            parts = parts.reshape(far, width, cols)
            parts = exchange(parts, far_groups)
            sums.append(jnp.sum(parts.astype(jnp.float32), axis=0))
    query_grad = jnp.concatenate(dqs, axis=1)
    kv_parts = []
    for g in range(kv_heads):
        own, away = sum_blocks(ids, returned[g], tok_count, tok_count * (1 if far == 2 else far))
        if far == 2:
            away = lax.ppermute(away, "kv", [(j + near, j) for j in range(near)])
            kv_parts.append(own + away.astype(jnp.float32))
        else:
            away = exchange(away.reshape(far, tok_count, ROW), far_groups)
            kv_parts.append(own + jnp.sum(away.astype(jnp.float32), axis=0))
    kv_grad = jnp.concatenate(kv_parts, axis=1)
    weight_grad = jnp.concatenate(sums, axis=1)
    return (query_grad, kv_grad, weight_grad)


def solution(mesh):
    in_specs = (
        P("kv", "tp"),
        P("kv", "tp"),
        P("kv", "tp"),
        P("kv", "tp"),
        P("kv", None),
        P("kv", None),
    )
    out_specs = (P("kv", "tp"), P("kv", "tp"), P("kv", "tp"))
    return jax.shard_map(shards, mesh=mesh, in_specs=in_specs, out_specs=out_specs, check_vma=False)
```

```python
import functools

import jax
import jax.numpy as jnp
from jax import lax
from jax.experimental import pallas as pl
from jax.experimental.pallas import tpu as pltpu
from jax.sharding import PartitionSpec as P


DH = 64
BLK = 64
QB = 128
NSEL = 16
ROW = 2 * DH


def attn_kernel(chosen_ref, slot_ref, first_ref, q_ref, o_ref, lse_ref, kv_ref, dq_ref, dqt_ref, tab_ref,
                x, xt, kvg, p_s, d_s, ds_s, acc, *, nsel, group, at, unroll, scale):
    i = pl.program_id(0)
    cols = group * QB
    pair = 2 * QB

    @pl.when(i == 0)
    def _():
        acc[...] = jnp.zeros_like(acc)
        x[...] = jnp.zeros_like(x)
        xt[...] = jnp.zeros_like(xt)

    gap = lax.broadcasted_iota(jnp.int32, (BLK, QB), 0) - lax.broadcasted_iota(
        jnp.int32, (BLK, QB), 1
    )

    def prepare(u):
        q = q_ref[pl.ds(u * QB, QB), :] * jnp.bfloat16(scale)
        o = o_ref[pl.ds(u * QB, QB), :]
        qt, ot = q.T, o.T
        for a in range(group):
            s = slice(a * DH, (a + 1) * DH)
            r = pl.ds(a * QB, QB)
            r2 = pl.ds(cols + a * QB, QB)
            x[u, r, pl.ds(0, DH)] = q[:, s]
            x[u, r2, pl.ds(DH, DH)] = o[:, s]
            xt[u, pl.ds(0, DH), r] = qt[s]
            xt[u, pl.ds(DH, DH), r2] = ot[s]
        block = i * unroll + u
        start = (first_ref[0] + block) * QB
        slots, limits = [], []
        for j in range(nsel):
            c = chosen_ref[block * nsel + j]
            slots.append(jnp.where(c >= 0, slot_ref[jnp.maximum(c, 0)], 0))
            limits.append(jnp.where(c >= 0, start - c * BLK, -(1 << 28)))
        for j in range(nsel):
            r = pl.ds(pl.multiple_of(slots[j] * BLK, BLK), BLK)
            kvg[u, pl.ds(j * BLK, BLK), :] = kv_ref[r, :]
        return slots, limits

    def scores(u, h, limits):
        top = lse_ref[at * group + 2 * h:at * group + 2 * h + 1, pl.ds(u * QB, QB)]
        low_row = lse_ref[at * group + 2 * h + 1:at * group + 2 * h + 2, pl.ds(u * QB, QB)]
        lse = jnp.concatenate([top, low_row], axis=1)
        here = pl.ds(h * pair, pair)
        there = pl.ds(cols + h * pair, pair)
        st = jnp.dot(kvg[u], xt[u, :, here], preferred_element_type=jnp.float32)
        dp = jnp.dot(kvg[u], xt[u, :, there], preferred_element_type=jnp.float32)
        part = jnp.zeros((8, pair), jnp.float32)
        for j in range(nsel):
            seen = gap <= limits[j]
            seen = jnp.concatenate([seen, seen], axis=1)
            sl = slice(j * BLK, (j + 1) * BLK)
            p = jnp.where(seen, jnp.exp(st[sl] - lse), 0.0)
            d = dp[sl]
            low = p.astype(jnp.bfloat16)
            prod = low.astype(jnp.float32) * d
            part = part + jnp.sum(prod.reshape(BLK // 8, 8, pair), axis=0)
            r = pl.ds(j * BLK, BLK)
            p_s[u, r, here] = p
            d_s[u, r, here] = d
            ds_s[u, r, there] = low
        return jnp.sum(part, axis=0, keepdims=True)

    def grads(u, slots, deltas):
        for h in range(cols // pair):
            here = pl.ds(h * pair, pair)
            ds_s[u, :, here] = (p_s[u, :, here] * (d_s[u, :, here] - deltas[h])).astype(jnp.bfloat16)
        kt = kvg[u].T[:DH]
        dqt = jnp.dot(kt, ds_s[u, :, pl.ds(0, cols)], preferred_element_type=jnp.float32)
        g = jnp.dot(ds_s[u], x[u], preferred_element_type=jnp.float32)
        for j in range(nsel):
            r = pl.ds(pl.multiple_of(slots[j] * BLK, BLK), BLK)
            acc[r, :] += g[j * BLK:(j + 1) * BLK]
        stack = jnp.concatenate([dqt[:, a * QB:(a + 1) * QB] for a in range(group)], axis=0)
        stack = scale * stack
        dqt_ref[:, pl.ds(u * QB, QB)] = stack.astype(dqt_ref.dtype)
        dq_ref[pl.ds(u * QB, QB), :] = stack.T.astype(dq_ref.dtype)

    blocks = [prepare(u) for u in range(unroll)]
    deltas = [[scores(u, h, blocks[u][1]) for h in range(cols // pair)] for u in range(unroll)]
    for u in range(unroll):
        grads(u, blocks[u][0], deltas[u])

    @pl.when(i == pl.num_programs(0) - 1)
    def _():
        tab_ref[...] = acc[...].astype(tab_ref.dtype)


def attn(chosen, slots, first, queries, out_grad, log_sums, kv, *, nsel, group, at):
    nq = queries.shape[0] // QB
    unroll = next(u for u in (3, 2, 1) if nq % u == 0)
    cols = group * QB
    rows = unroll * QB
    wide = pl.BlockSpec((rows, group * DH), lambda i, *_: (i, at))
    return pl.pallas_call(
        functools.partial(
            attn_kernel, nsel=nsel, group=group, at=at, unroll=unroll, scale=DH ** (-0.5)
        ),
        grid_spec=pltpu.PrefetchScalarGridSpec(
            num_scalar_prefetch=3,
            grid=(nq // unroll,),
            in_specs=[
                wide,
                wide,
                pl.BlockSpec((log_sums.shape[0], rows), lambda i, *_: (0, i)),
                pl.BlockSpec(kv.shape, lambda i, *_: (0, 0)),
            ],
            out_specs=[
                pl.BlockSpec((rows, group * DH), lambda i, *_: (i, 0)),
                pl.BlockSpec((group * DH, rows), lambda i, *_: (0, i)),
                pl.BlockSpec(kv.shape, lambda i, *_: (0, 0)),
            ],
            scratch_shapes=[
                pltpu.VMEM((unroll, 2 * cols, ROW), jnp.bfloat16),
                pltpu.VMEM((unroll, ROW, 2 * cols), jnp.bfloat16),
                pltpu.VMEM((unroll, nsel * BLK, ROW), jnp.bfloat16),
                pltpu.VMEM((unroll, nsel * BLK, cols), jnp.float32),
                pltpu.VMEM((unroll, nsel * BLK, cols), jnp.float32),
                pltpu.VMEM((unroll, nsel * BLK, 2 * cols), jnp.bfloat16),
                pltpu.VMEM(kv.shape, jnp.float32),
            ],
        ),
        out_shape=[
            jax.ShapeDtypeStruct((nq * QB, group * DH), jnp.bfloat16),
            jax.ShapeDtypeStruct((group * DH, nq * QB), jnp.bfloat16),
            jax.ShapeDtypeStruct(kv.shape, jnp.bfloat16),
        ],
        compiler_params=pltpu.CompilerParams(dimension_semantics=("arbitrary",)),
        cost_estimate=pl.CostEstimate(
            flops=nq * nsel * BLK * ROW * cols * 10,
            bytes_accessed=4 * kv.size + 8 * nq * QB * group * DH,
            transcendentals=nq * nsel * BLK * cols,
        ),
        name="attn_bwd",
    )(chosen, slots, first, queries, out_grad, log_sums, kv)


def pick_kernel(ids_ref, own_ref, away_ref, out_ref):
    edge = own_ref.shape[0] // BLK
    for j in range(out_ref.shape[0] // BLK):
        at = jnp.maximum(ids_ref[j], 0)

        @pl.when(at < edge)
        def _(j=j, at=at):
            r = pl.ds(pl.multiple_of(at * BLK, BLK), BLK)
            out_ref[pl.ds(j * BLK, BLK), :] = own_ref[r, :]

        @pl.when(at >= edge)
        def _(j=j, at=at):
            r = pl.ds(pl.multiple_of((at - edge) * BLK, BLK), BLK)
            out_ref[pl.ds(j * BLK, BLK), :] = away_ref[r, :]


def pick_blocks(ids, own, away):
    vmem = pl.BlockSpec(memory_space=pltpu.VMEM)
    return pl.pallas_call(
        pick_kernel,
        in_specs=[pl.BlockSpec(memory_space=pltpu.SMEM), vmem, vmem],
        out_specs=vmem,
        out_shape=jax.ShapeDtypeStruct((ids.shape[0] * BLK, own.shape[1]), own.dtype),
        name="pick_blocks",
    )(ids, own, away)


def sum_kernel(ids_ref, in_ref, own_ref, away_ref, acc):
    edge = own_ref.shape[0]
    acc[...] = jnp.zeros_like(acc)
    for j in range(in_ref.shape[0] // BLK):
        at = ids_ref[j]

        @pl.when(at >= 0)
        def _(j=j, at=at):
            r = pl.ds(pl.multiple_of(at * BLK, BLK), BLK)
            acc[r, :] += in_ref[pl.ds(j * BLK, BLK), :].astype(jnp.float32)

    own_ref[...] = acc[pl.ds(0, edge), :]
    away_ref[...] = acc[pl.ds(edge, away_ref.shape[0]), :].astype(away_ref.dtype)


def sum_blocks(ids, back, own_rows, away_rows):
    vmem = pl.BlockSpec(memory_space=pltpu.VMEM)
    width = back.shape[1]
    return pl.pallas_call(
        sum_kernel,
        in_specs=[pl.BlockSpec(memory_space=pltpu.SMEM), vmem],
        out_specs=[vmem, vmem],
        out_shape=[
            jax.ShapeDtypeStruct((own_rows, width), jnp.float32),
            jax.ShapeDtypeStruct((away_rows, width), jnp.bfloat16),
        ],
        scratch_shapes=[pltpu.VMEM((own_rows + away_rows, width), jnp.float32)],
        name="sum_blocks",
    )(ids, back)


def pack_kernel(*refs):
    n = (len(refs) - 3)
    sources, out_ref = refs[:n], refs[n]
    buf, sems = refs[n + 1:]
    tok = buf.shape[1]
    ins = [pltpu.make_async_copy(sources[k], buf.at[k], sems.at[k]) for k in range(n)]
    outs = [
        pltpu.make_async_copy(buf.at[k], out_ref.at[pl.ds(k * tok, tok), :], sems.at[n + k])
        for k in range(n)
    ]
    for copy in ins:
        copy.start()
    for k in range(n):
        ins[k].wait()
        outs[k].start()
    for copy in outs:
        copy.wait()


def pack(parts):
    hbm = pl.BlockSpec(memory_space=pl.ANY)
    n = len(parts)
    shape = (parts[0].shape[0] * n, parts[0].shape[1])
    return pl.pallas_call(
        pack_kernel,
        in_specs=[hbm] * n,
        out_specs=hbm,
        out_shape=jax.ShapeDtypeStruct(shape, parts[0].dtype),
        scratch_shapes=[
            pltpu.VMEM((n,) + parts[0].shape, parts[0].dtype),
            pltpu.SemaphoreType.DMA((2 * n,)),
        ],
        name="pack",
    )(*parts)


def weight_kernel(place_ref, inputs_ref, *refs, near, pieces):
    sources = refs[:4 + near]
    own_ref, other_ref, rows_t, quarters, sems = refs[4 + near:]
    tok = rows_t.shape[1] // near
    size = sources[0].shape[1]
    copies = [
        pltpu.make_async_copy(sources[4 + k], rows_t.at[:, pl.ds(k * tok, tok)], sems.at[k])
        for k in range(near)
    ]
    local, rest = [], []
    for k in range(4):
        for f in range(pieces):
            col = pl.ds(pl.multiple_of(place_ref[2 + k * pieces + f], 128), size // pieces)
            to = quarters.at[pl.ds(0, tok), pl.ds(k * size + f * (size // pieces), size // pieces)]
            at = near + 4 + k * pieces + f
            local.append(pltpu.make_async_copy(inputs_ref.at[:, col], to, sems.at[at]))
        to = quarters.at[pl.ds(tok, (near - 1) * tok), pl.ds(k * size, size)]
        rest.append(pltpu.make_async_copy(sources[k], to, sems.at[near + k]))
    for copy in copies:
        copy.start()
    for k in range(4):
        for copy in local[k * pieces:(k + 1) * pieces]:
            copy.start()
        rest[k].start()
    for copy in copies:
        copy.wait()
    core, chip = place_ref[0], place_ref[1]
    for pair in range(2):
        for k in (2 * pair, 2 * pair + 1):
            rest[k].wait()
            for copy in local[k * pieces:(k + 1) * pieces]:
                copy.wait()
        both = jnp.dot(
            rows_t[...],
            quarters[:, pl.ds(pair * 2 * size, 2 * size)],
            preferred_element_type=jnp.float32,
        )
        away = core if pair == 0 else 1 - core
        for k in range(2):
            t = both[:, k * size:(k + 1) * size].T
            sub = chip if k == 0 else 1 - chip
            at = pl.ds(pl.multiple_of(sub * size, size), size)

            @pl.when(away == 0)
            def _(t=t, at=at):
                own_ref[at, :] = t

            @pl.when(away == 1)
            def _(t=t, at=at):
                other_ref[at, :] = t.astype(other_ref.dtype)


def weight_parts(place, inputs, quarters, parts):
    vmem = pl.BlockSpec(memory_space=pltpu.VMEM)
    near = len(parts)
    cols, tok = parts[0].shape
    size = quarters[0].shape[1]
    pieces = (place.shape[0] - 2) // 4
    flops = 2 * near * tok * cols * 4 * size
    return pl.pallas_call(
        functools.partial(weight_kernel, near=near, pieces=pieces),
        in_specs=[pl.BlockSpec(memory_space=pltpu.SMEM)]
        + [pl.BlockSpec(memory_space=pl.ANY)] * (5 + near),
        out_specs=[vmem, vmem],
        out_shape=[
            jax.ShapeDtypeStruct((2 * size, cols), jnp.float32),
            jax.ShapeDtypeStruct((2 * size, cols), jnp.bfloat16),
        ],
        scratch_shapes=[
            pltpu.VMEM((cols, near * tok), jnp.bfloat16),
            pltpu.VMEM((near * tok, 4 * size), jnp.bfloat16),
            pltpu.SemaphoreType.DMA((near + 4 + 4 * pieces,)),
        ],
        cost_estimate=pl.CostEstimate(
            flops=flops, bytes_accessed=2 * 6 * quarters[0].size, transcendentals=0
        ),
        name="weight_parts",
    )(place, inputs, *quarters, *parts)


def exchange(x, groups):
    return lax.all_to_all(
        x, "kv", split_axis=0, concat_axis=0, tiled=True, axis_index_groups=groups
    )


def hop(x, step, axis="kv"):
    n = lax.axis_size(axis)
    return lax.ppermute(x, axis, [(j, j ^ step) for j in range(n)])


def column_starts(width, near, far, here, core, chip):
    half = far // 2
    side = ((lax.axis_index("kv") // near) % 2) ^ core
    if half == 1:
        return [(side * near + here) * width + chip * (width // 2)], width // 2
    owners = [side * half + chip * (half // 2) + f for f in range(half // 2)]
    return [(owner * near + here) * width for owner in owners], width


def input_slices(inputs, near, far):
    tok = inputs.shape[0]
    width = inputs.shape[1] // (near * far)
    here, at = lax.axis_index("kv") % near, lax.axis_index("tp")
    slices = []
    for step in range(1, near):
        cols, size = column_starts(width, near, far, here ^ step, at % 2, (at // 2) % 2)
        parts = [lax.dynamic_slice(inputs, (0, col), (tok, size)) for col in cols]
        slices.append(parts[0] if len(parts) == 1 else jnp.concatenate(parts, axis=1))
    return slices


def shards(queries, keys_values, log_sums, out_grad, inputs, chosen):
    tok_count = queries.shape[0]
    heads_here = queries.shape[1] // DH
    kv_heads = keys_values.shape[1] // ROW
    group = heads_here // kv_heads
    blocks_here = tok_count // BLK
    query_blocks = tok_count // QB
    kv_count = lax.axis_size("kv")
    near = 4
    far = kv_count // near
    me = lax.axis_index("kv")
    first_block = me * query_blocks
    capacity = blocks_here // 2
    total_blocks = kv_count * blocks_here

    flat_ids = chosen.reshape(-1)
    needed = jnp.any(
        flat_ids[:, None] == jnp.arange(total_blocks, dtype=jnp.int32)[None, :], axis=0
    )
    needed = needed.reshape(kv_count, blocks_here).astype(jnp.int32)
    rank_in = jnp.cumsum(needed, axis=1) - 1
    matches = (needed[:, :, None] == 1) & (
        rank_in[:, :, None] == jnp.arange(capacity, dtype=jnp.int32)[None, None, :]
    )
    request = jnp.sum(
        matches.astype(jnp.int32) * jnp.arange(blocks_here, dtype=jnp.int32)[None, :, None], axis=1
    )
    request = jnp.where(jnp.any(matches, axis=1), request, -1)
    request = jnp.swapaxes(request.reshape(far, near, capacity), 0, 1)
    near_groups = [[f * near + d for d in range(near)] for f in range(far)]
    far_groups = [[f * near + d for f in range(far)] for d in range(near)]
    far_at = me // near

    slices = input_slices(inputs, near, far)
    heads_kv = [keys_values[:, g * ROW : (g + 1) * ROW] for g in range(kv_heads)]
    away_kv = []
    for g in range(kv_heads):
        if far == 2:
            away_kv.append(lax.ppermute(heads_kv[g], "kv", [(j, j + near) for j in range(near)]))
        else:
            away_kv.append(
                lax.all_gather(heads_kv[g], "kv", tiled=True, axis_index_groups=far_groups)
            )
    asked = exchange(request, near_groups)
    owner = jnp.arange(far, dtype=jnp.int32)
    offset = ((owner != far_at) if far == 2 else owner + 1).astype(jnp.int32) * blocks_here
    ids = jnp.where(asked >= 0, asked + offset[None, :, None], -1).reshape(-1)
    of_block = jnp.arange(total_blocks, dtype=jnp.int32) // blocks_here
    slots = ((of_block % near) * far + of_block // near) * capacity + rank_in.reshape(-1)
    slots = jnp.clip(slots, 0, kv_count * capacity - 1)
    first = first_block.astype(jnp.int32).reshape(1)
    flat_chosen = chosen.reshape(-1)
    lse = log_sums.T

    tables = []
    for g in range(kv_heads):
        send = pick_blocks(ids, heads_kv[g], away_kv[g])
        table = exchange(send.reshape(near, -1, ROW), near_groups)
        tables.append(table.reshape(kv_count * capacity * BLK, ROW))
    got = []
    for step in range(1, near):
        got.append(hop(slices[step - 1], step))

    dqs, returned, sums = [], [], []
    nears = []
    for g in range(kv_heads):
        dq, dqt, tab = attn(
            flat_chosen, slots, first, queries, out_grad, lse, tables[g],
            nsel=NSEL, group=group, at=g,
        )
        dqs.append(dq)
        nears.append([dqt])
        for step in range(1, near):
            relay = step == 3
            nears[g].append(hop(nears[g][2], 1) if relay else hop(dqt, step))
        back = exchange(tab.reshape(near, -1, ROW), near_groups)
        returned.append(back.reshape(kv_count * capacity * BLK, ROW))
    seen = pack(got)
    beside = hop(seen, 2, "tp")
    twin = hop(seen, 1, "tp")
    beside_twin = hop(beside, 1, "tp")
    quarters = (seen, beside, twin, beside_twin)
    at = lax.axis_index("tp").astype(jnp.int32)
    core, chip = at % 2, (at // 2) % 2
    width = inputs.shape[1] // kv_count
    entries = [core, chip]
    for k in range(4):
        cols, _ = column_starts(width, near, far, me % near, core ^ (k // 2), chip ^ (k % 2))
        entries += cols
    place = jnp.stack([jnp.asarray(e, jnp.int32) for e in entries])
    for g in range(kv_heads):
        own, other = weight_parts(place, inputs, quarters, nears[g])
        cols = own.shape[1]
        if far == 2:
            other = hop(other, near)
            sums.append(own + other.astype(jnp.float32))
        else:
            even = (me // near) % 2 == 0
            own = own.astype(jnp.bfloat16)
            parts = jnp.concatenate([jnp.where(even, own, other), jnp.where(even, other, own)], axis=0)
            parts = parts.reshape(far, width, cols)
            parts = exchange(parts, far_groups)
            sums.append(jnp.sum(parts.astype(jnp.float32), axis=0))
    query_grad = jnp.concatenate(dqs, axis=1)
    kv_parts = []
    for g in range(kv_heads):
        own, away = sum_blocks(ids, returned[g], tok_count, tok_count * (1 if far == 2 else far))
        if far == 2:
            away = lax.ppermute(away, "kv", [(j + near, j) for j in range(near)])
            kv_parts.append(own + away.astype(jnp.float32))
        else:
            away = exchange(away.reshape(far, tok_count, ROW), far_groups)
            kv_parts.append(own + jnp.sum(away.astype(jnp.float32), axis=0))
    kv_grad = jnp.concatenate(kv_parts, axis=1)
    weight_grad = jnp.concatenate(sums, axis=1)
    return (query_grad, kv_grad, weight_grad)


def solution(mesh):
    in_specs = (
        P("kv", "tp"),
        P("kv", "tp"),
        P("kv", "tp"),
        P("kv", "tp"),
        P("kv", None),
        P("kv", None),
    )
    out_specs = (P("kv", "tp"), P("kv", "tp"), P("kv", "tp"))
    return jax.shard_map(shards, mesh=mesh, in_specs=in_specs, out_specs=out_specs, check_vma=False)
```
